256 devices in a mesh: fs: 64 (over z, y, core), tp: 4 (over x).
Axes of the slice: x: 4, y: 4, z: 8, core: 2. Of those that a mesh axis runs over, the one named last changes fastest.
Arguments:
- tokens: bfloat16 [65536, 2048], P('fs', 'tp'), may hold values from -6 to 6
- norm_gain: float32 [2048], P('fs'), may hold values from 0.1 to 1.9
- up_master: float32 [2048, 4096], P('fs', 'tp'), may hold values from -0.125 to 0.125
- down_master: float32 [4096, 2048], P('fs', 'tp'), may hold values from -0.09375 to 0.09375
Outputs:
- mixed: bfloat16 [65536, 2048], P('fs', 'tp')
- up_ready: bfloat16 [2048, 4096], P(None, 'tp')
- down_ready: bfloat16 [4096, 2048], P('tp')
The draws below stay inside these ranges and needn't reach their ends.
All inputs are finite; a program needn't handle non-finite values.
Results may differ from the reference program's by a relative error of at most 0.0095.
Values may be sent and summed in bfloat16 or wider, within the bound.
A program may use at most 128 MiB of HBM per device.

```python
import jax
import jax.numpy as jnp
from jax import lax

D = 2048
FF = 4096
TOKENS = 65536
N_TP = 4


def steps_of(key, shape, shards, least, high):
    factor_of, own = 1.0, jax.random.fold_in(key, 6)
    for axis_at, blocks in shards:
        steps = jnp.exp(jax.random.uniform(jax.random.fold_in(own, axis_at), (blocks,), jnp.float32, least / len(shards), high / len(shards)))
        factor_of = factor_of * jnp.repeat(steps, shape[axis_at] // blocks).reshape([-1 if axis == axis_at else 1 for axis in range(len(shape))])
    return factor_of


def gaussian(rng, dims, spread, bound, pieces=(), held_as=jnp.bfloat16):
    loudness = steps_of(rng, dims, pieces, -0.22, 0.18) if pieces else 1.0
    array = jax.random.normal(rng, dims, jnp.float32) * spread * loudness
    return jnp.minimum(jnp.maximum(array, -bound), bound).astype(held_as)


def setup_inputs(seed: int = 0) -> dict:
    arg_keys = jax.random.split(jax.random.key(seed), 5)
    tokens = gaussian(arg_keys[0], (TOKENS, D), 1.0, 6.0, ((0, 64), (1, 4)))
    norm_gain = jnp.clip(1.0 + 0.18 * jax.random.normal(arg_keys[1], (D,), jnp.float32), 0.1, 1.9)
    up_master = gaussian(arg_keys[2], (D, FF), D ** -0.5, 0.125, ((0, 64), (1, 4)), jnp.float32)
    down_master = gaussian(arg_keys[3], (FF, D), FF ** -0.5, 0.09375, ((0, 64), (1, 4)), jnp.float32)
    return {"tokens": tokens, "norm_gain": norm_gain, "up_master": up_master, "down_master": down_master}


def reference(tokens, norm_gain, up_master, down_master):
    up_ready = (norm_gain[:, None] * up_master).astype(jnp.bfloat16)
    down_ready = down_master.astype(jnp.bfloat16)
    values = tokens.astype(jnp.float32)
    mean_square = lax.optimization_barrier(jnp.mean(values * values, axis=-1, keepdims=True))
    normed = (values * lax.rsqrt(mean_square + 1e-06)).astype(jnp.bfloat16)
    before = jnp.dot(normed, up_ready, preferred_element_type=jnp.float32)
    hidden = jnp.square(jax.nn.relu(before)).astype(jnp.bfloat16)
    block_size = FF // N_TP
    total = jnp.zeros((tokens.shape[0], D), jnp.float32)
    for block_id in range(N_TP):
        first = block_id * block_size
        partial_value = jnp.dot(hidden[:, first:first + block_size], down_ready[first:first + block_size], preferred_element_type=jnp.float32).astype(jnp.bfloat16)
        partial_value = lax.optimization_barrier(partial_value)
        total = total + partial_value.astype(jnp.float32)
    return (total.astype(jnp.bfloat16), up_ready, down_ready)
```

```python
import functools

import jax
import jax.numpy as jnp
from jax import lax
from jax.experimental import pallas as pl
from jax.experimental.pallas import tpu as pltpu
from jax.sharding import Mesh
from jax.sharding import PartitionSpec as P

FS = ("z", "y", "c")
NZ, NY, NC, NX = 8, 4, 2, 4
CHUNKS = 4
ROWS = 256
MESH = pl.DeviceIdType.MESH


def kernel(
    tok_ref, gain_ref, up_ref, down_ref,
    mixed_ref, up_out, down_out,
    U, D, dl, X, N, H, PT, R2, RA, RB, MX,
    loc_sem, out_sem, dsc_sem,
    uz_s, uz_r, uy_s, uy_r, up_s, up_r,
    dz_s, dz_r, dy_s, dy_r, dp_s, dp_r,
    tx_s, tx_r, rs_s, rs_r,
):
    x, y, z, c = (lax.axis_index(a) for a in ("x", "y", "z", "c"))
    s = 1 - 2 * c

    def xo(k):
        return lax.rem(x + k * s + 2 * NX, NX)

    def yo(k):
        return lax.rem(y + k * s + 2 * NY, NY)

    def zo(k):
        return lax.rem(z + k * s + 2 * NZ, NZ)

    sent = []

    def send(src, dst, ssem, rsem, dev):
        copy = pltpu.make_async_remote_copy(
            src_ref=src, dst_ref=dst, send_sem=ssem, recv_sem=rsem,
            device_id=dev, device_id_type=MESH,
        )
        copy.start()
        sent.append(copy)

    def arrive(dst, ssem, rsem, dev):
        pltpu.make_async_remote_copy(
            src_ref=dst, dst_ref=dst, send_sem=ssem, recv_sem=rsem,
            device_id=dev, device_id_type=MESH,
        ).wait_recv()

    xp, xm = {"x": xo(1)}, {"x": xo(-1)}
    yp, ym = {"y": yo(1)}, {"y": yo(-1)}
    zp, zm = {"z": zo(1)}, {"z": zo(-1)}
    mate = {"c": 1 - c}
    block = lax.div(z, 2)
    far_z = 2 * x + lax.rem(z, 2)
    turned = {"x": block, "z": far_z}
    away = x != block

    load = pltpu.make_async_copy(tok_ref, X.at[3], loc_sem)
    load.start()

    barrier = pltpu.get_barrier_semaphore()
    for dev in (xp, xm, yp, ym, zp, zm, mate):
        pl.semaphore_signal(barrier, inc=1, device_id=dev, device_id_type=MESH)

    @pl.when(away)
    def _():
        pl.semaphore_signal(barrier, inc=1, device_id=turned, device_id_type=MESH)

    gain = gain_ref[...]
    eye = lax.broadcasted_iota(jnp.int32, (32, 32), 0) == lax.broadcasted_iota(jnp.int32, (32, 32), 1)
    column = jnp.sum(jnp.where(eye, jnp.broadcast_to(gain, (32, 32)), 0.0), axis=1, keepdims=True)
    U[z, y, c] = (column * up_ref[...]).astype(jnp.bfloat16)
    mine = down_ref[...].astype(jnp.bfloat16)
    dl[...] = mine

    @pl.when(jnp.logical_not(away))
    def _():
        D[z, y, c] = mine

    load.wait()

    @pl.when(away)
    def _():
        pl.semaphore_wait(barrier, 8)

    @pl.when(jnp.logical_not(away))
    def _():
        pl.semaphore_wait(barrier, 7)

    def rows(i):
        return pl.ds(i * ROWS, ROWS)

    scatter = pltpu.make_async_remote_copy(
        src_ref=dl, dst_ref=D.at[far_z, y, c], send_sem=dsc_sem.at[0], recv_sem=dsc_sem.at[1],
        device_id=turned, device_id_type=MESH,
    )

    @pl.when(away)
    def _():
        scatter.start()

    u_own = U.at[z, y, c]
    send(u_own, u_own, uz_s.at[0], uz_r.at[0], zp)
    send(u_own, u_own, uz_s.at[4], uz_r.at[4], zm)
    for i in range(CHUNKS):
        send(X.at[3, rows(i)], X.at[0, rows(i)], tx_s.at[0, i], tx_r.at[0, i], xp)
        send(X.at[3, rows(i)], X.at[1, rows(i)], tx_s.at[1, i], tx_r.at[1, i], xm)

    events = []

    def at(time, fn):
        events.append((time, len(events), fn))

    z_offsets = [0, -1, 1, -2, 2, -3, 3, -4]

    def u_row(n):
        zz = zo(z_offsets[n])
        piece = U.at[zz, y, c]
        send(piece, piece, uy_s.at[n, 0], uy_r.at[n, 0], yp)
        send(piece, piece, uy_s.at[n, 1], uy_r.at[n, 1], ym)

    def u_z(n):
        k = z_offsets[n]
        piece = U.at[zo(k), y, c]
        if k < 0:
            arrive(piece, uz_s.at[-k - 1], uz_r.at[-k - 1], zm)
            if k > -4:
                send(piece, piece, uz_s.at[-k], uz_r.at[-k], zp)
        else:
            arrive(piece, uz_s.at[3 + k], uz_r.at[3 + k], zp)
            if k < 3:
                send(piece, piece, uz_s.at[4 + k], uz_r.at[4 + k], zm)
        u_row(n)

    def u_y1(n):
        zz = zo(z_offsets[n])
        left = U.at[zz, yo(-1), c]
        arrive(left, uy_s.at[n, 0], uy_r.at[n, 0], ym)
        send(left, left, uy_s.at[n, 2], uy_r.at[n, 2], yp)
        arrive(U.at[zz, yo(1), c], uy_s.at[n, 1], uy_r.at[n, 1], yp)

    def u_y2(n):
        zz = zo(z_offsets[n])
        arrive(U.at[zz, yo(-2), c], uy_s.at[n, 2], uy_r.at[n, 2], ym)
        full = U.at[zz, :, c]
        send(full, full, up_s.at[zz], up_r.at[zz], mate)

    u_row(0)
    u_tz = [0, 3.2, 3.2, 6.4, 6.4, 9.6, 9.6, 12.8]
    u_t1 = [3.3, 6.8, 7.0, 10.8, 11.0, 14.8, 15.0, 18.0]
    for n in range(NZ):
        if n:
            at(u_tz[n], functools.partial(u_z, n))
        at(u_t1[n], functools.partial(u_y1, n))
        at(u_t1[n] + 3.1, functools.partial(u_y2, n))

    y_offsets = [0, -1, 1, -2]

    def d_row(m):
        piece = D.at[z, yo(y_offsets[m]), c]
        send(piece, piece, dz_s.at[m, 0], dz_r.at[m, 0], zm)
        send(piece, piece, dz_s.at[m, 4], dz_r.at[m, 4], zp)

    def d_own():
        @pl.when(away)
        def _():
            scatter.wait_recv()

        piece = D.at[z, y, c]
        send(piece, piece, dy_s.at[0], dy_r.at[0], yp)
        send(piece, piece, dy_s.at[1], dy_r.at[1], ym)
        d_row(0)

    def d_y1():
        left = D.at[z, yo(-1), c]
        arrive(left, dy_s.at[0], dy_r.at[0], ym)
        send(left, left, dy_s.at[2], dy_r.at[2], yp)
        d_row(1)
        arrive(D.at[z, yo(1), c], dy_s.at[1], dy_r.at[1], yp)
        d_row(2)

    def d_y2():
        arrive(D.at[z, yo(-2), c], dy_s.at[2], dy_r.at[2], ym)
        d_row(3)
        full = D.at[z, :, c]
        send(full, full, dp_s.at[z], dp_r.at[z], mate)

    def d_z(m, k):
        yy = yo(y_offsets[m])
        piece = D.at[zo(k), yy, c]
        if k > 0:
            arrive(piece, dz_s.at[m, k - 1], dz_r.at[m, k - 1], zp)
            if k < 4:
                send(piece, piece, dz_s.at[m, k], dz_r.at[m, k], zm)
        else:
            arrive(piece, dz_s.at[m, 3 - k], dz_r.at[m, 3 - k], zm)
            if k > -3:
                send(piece, piece, dz_s.at[m, 4 - k], dz_r.at[m, 4 - k], zp)
        if m == 3:
            full = D.at[zo(k), :, c]
            send(full, full, dp_s.at[zo(k)], dp_r.at[zo(k)], mate)

    at(5.0, d_own)
    at(9.0, d_y1)
    at(12.2, d_y2)
    d_t = [[8.4, 11.8, 15.2, 18.6], [12.6, 16.4, 20.2, 24.0], [12.8, 16.6, 20.4, 24.2], [15.8, 20.0, 24.6, 28.0]]
    for m in range(NY):
        for k in (1, 2, 3, 4):
            at(d_t[m][k - 1], functools.partial(d_z, m, k))
            if k < 4:
                at(d_t[m][k - 1] + 0.1, functools.partial(d_z, m, -k))

    def x_near(i):
        arrive(X.at[0, rows(i)], tx_s.at[0, i], tx_r.at[0, i], xm)
        send(X.at[0, rows(i)], X.at[2, rows(i)], tx_s.at[2, i], tx_r.at[2, i], xp)

    for i in range(CHUNKS):
        at(7.3 + 5.6 * i, functools.partial(x_near, i))

    for _, _, fn in sorted(events, key=lambda e: e[:2]):
        fn()

    def normalise(i):
        arrive(X.at[1, rows(i)], tx_s.at[1, i], tx_r.at[1, i], xp)
        arrive(X.at[2, rows(i)], tx_s.at[2, i], tx_r.at[2, i], xm)
        owners = (xo(-1), xo(1), xo(2), x)

        @pl.loop(0, ROWS // 32)
        def _(b):
            r = pl.ds(pl.multiple_of(i * ROWS + b * 32, 32), 32)
            values = [X[n, r, :].astype(jnp.float32) for n in range(4)]
            total = sum(jnp.sum(v * v, axis=1, keepdims=True) for v in values)
            scale = lax.rsqrt(total * (1.0 / 2048) + 1e-6)
            for v, owner in zip(values, owners):
                N[r, pl.ds(pl.multiple_of(owner * 512, 512), 512)] = (v * scale).astype(jnp.bfloat16)

    def first(i):
        for n in range(4):
            w = U[:, :, :, :, n * 256:(n + 1) * 256].reshape(2048, 256)
            before = jnp.dot(N[rows(i), :], w, preferred_element_type=jnp.float32)
            before = jnp.maximum(before, 0.0)
            H[:, n * 256:(n + 1) * 256] = (before * before).astype(jnp.bfloat16)

    def second(i):
        for j, (k, buf, sem, dev) in enumerate(((2, R2, 0, xp), (-1, RB, 1, xm), (1, None, 2, None), (0, None, 3, None))):
            cc = xo(k)
            w = D[pl.ds(2 * cc, 2)].reshape(1024, 512)
            PT[i, j] = jnp.dot(H[...], w, preferred_element_type=jnp.float32).astype(jnp.bfloat16)
            if buf is not None:
                send(PT.at[i, j], buf.at[i], rs_s.at[sem, i], rs_r.at[sem, i], dev)

    def relay(i):
        arrive(R2.at[i], rs_s.at[0, i], rs_r.at[0, i], xm)
        PT[i, 2] = (PT[i, 2].astype(jnp.float32) + R2[i].astype(jnp.float32)).astype(jnp.bfloat16)
        send(PT.at[i, 2], RA.at[i], rs_s.at[2, i], rs_r.at[2, i], xp)

    stores = []

    def finish(i):
        arrive(RB.at[i], rs_s.at[1, i], rs_r.at[1, i], xp)
        arrive(RA.at[i], rs_s.at[2, i], rs_r.at[2, i], xm)
        total = PT[i, 3].astype(jnp.float32) + RA[i].astype(jnp.float32) + RB[i].astype(jnp.float32)
        MX[rows(i), :] = total.astype(jnp.bfloat16)
        store = pltpu.make_async_copy(MX.at[rows(i)], mixed_ref.at[rows(i)], out_sem.at[i])
        store.start()
        stores.append(store)

    normalise(0)
    for n in range(NZ):
        full = U.at[n, :, 1 - c]
        arrive(full, up_s.at[n], up_r.at[n], mate)
    store = pltpu.make_async_copy(U, up_out, out_sem.at[4])
    store.start()
    stores.append(store)
    first(0)
    for n in range(NZ):
        full = D.at[n, :, 1 - c]
        arrive(full, dp_s.at[n], dp_r.at[n], mate)
    for n in range(NX):
        store = pltpu.make_async_copy(
            D.at[pl.ds(2 * n, 2)], down_out.at[:, :, :, :, pl.ds(n * 512, 512)], out_sem.at[5 + n]
        )
        store.start()
        stores.append(store)
    second(0)
    for i in range(1, CHUNKS):
        normalise(i)
        first(i)
        second(i)
        relay(i - 1)
        if i > 1:
            finish(i - 2)
    relay(CHUNKS - 1)
    finish(CHUNKS - 2)
    finish(CHUNKS - 1)

    for copy in sent:
        copy.wait_send()

    @pl.when(away)
    def _():
        scatter.wait_send()

    for store in stores:
        store.wait()


def shards(tokens, norm_gain, up_master, down_master):
    bf = jnp.bfloat16
    sem = pltpu.SemaphoreType.DMA
    vmem = pl.BlockSpec(memory_space=pltpu.VMEM)
    hbm = pl.BlockSpec(memory_space=pl.ANY)
    mixed, up, down = pl.pallas_call(
        kernel,
        out_shape=(
            jax.ShapeDtypeStruct((1024, 512), bf),
            jax.ShapeDtypeStruct((NZ, NY, NC, 32, 1024), bf),
            jax.ShapeDtypeStruct((2, NY, NC, 64, 2048), bf),
        ),
        in_specs=[hbm, vmem, vmem, vmem],
        out_specs=(hbm, hbm, hbm),
        scratch_shapes=[
            pltpu.VMEM((NZ, NY, NC, 32, 1024), bf),
            pltpu.VMEM((NZ, NY, NC, 64, 512), bf),
            pltpu.VMEM((64, 512), bf),
            pltpu.VMEM((4, 1024, 512), bf),
            pltpu.VMEM((1024, 2048), bf),
            pltpu.VMEM((ROWS, 1024), bf),
            pltpu.VMEM((CHUNKS, 4, ROWS, 512), bf),
            pltpu.VMEM((CHUNKS, ROWS, 512), bf),
            pltpu.VMEM((CHUNKS, ROWS, 512), bf),
            pltpu.VMEM((CHUNKS, ROWS, 512), bf),
            pltpu.VMEM((1024, 512), bf),
            sem, sem((9,)), sem((2,)),
            sem((7,)), sem((7,)), sem((8, 3)), sem((8, 3)), sem((8,)), sem((8,)),
            sem((4, 7)), sem((4, 7)), sem((3,)), sem((3,)), sem((8,)), sem((8,)),
            sem((3, CHUNKS)), sem((3, CHUNKS)), sem((3, CHUNKS)), sem((3, CHUNKS)),
        ],
        compiler_params=pltpu.CompilerParams(
            collective_id=0, has_side_effects=True, vmem_limit_bytes=48 * 1024 * 1024
        ),
        name="handoff",
    )(tokens, norm_gain.reshape(1, 32), up_master, down_master)
    return mixed, up.reshape(2048, 1024), down.reshape(1024, 2048)


def solution(mesh):
    finer = Mesh(mesh.devices.reshape(NZ, NY, NC, NX), ("z", "y", "c", "x"))
    return jax.shard_map(
        shards,
        mesh=finer,
        in_specs=(P(FS, "x"), P(FS), P(FS, "x"), P(FS, "x")),
        out_specs=(P(FS, "x"), P(None, "x"), P("x", None)),
        check_vma=False,
    )
```

```python
import jax
import jax.numpy as jnp
from jax import lax
from jax.experimental import pallas as pl
from jax.experimental.pallas import tpu as pltpu
from jax.sharding import Mesh
from jax.sharding import PartitionSpec as P

FS = ("z", "y", "c")
SIZE = {"z": 8, "y": 4, "c": 2, "x": 4}
CHUNKS = 4
ROWS = 256
MESH = pl.DeviceIdType.MESH
WAY = {("y", 1): (0, -1, 1, -2), ("z", 1): (0, -1, 1, -2, 2, -3, 3, -4), ("z", -1): (0, 1, -1, 2, -2, 3, -3, 4), ("y", -1): (0, 1, -1, 2)}
OWN, RING1, RING2, ROW, PASS, NORM, FIRST, SECOND, RELAY, FINISH = range(10)
UP_ORDER = (
    (OWN,), (RING1, -1), (RING1, 1), (RING2, 0, -1), (RING2, 0, 1), (PASS, 0), (RING1, -2), (RING2, 1, -1),
    (RING2, 1, 1), (RING1, 2), (RING2, 2, 1), (RING2, 2, -1), (RING2, 0, -2), (ROW, 0), (RING1, -3), (RING1, 3),
    (RING2, 3, 1), (PASS, 1), (RING2, 3, -1), (RING2, 4, 1), (RING2, 1, -2), (ROW, 1), (RING2, 4, -1), (RING2, 2, 2),
    (ROW, 2), (RING1, -4), (RING2, 5, -1), (RING2, 5, 1), (PASS, 2), (RING2, 6, -1), (RING2, 6, 1), (RING2, 4, -2),
    (ROW, 4), (RING2, 3, 2), (ROW, 3), (RING2, 7, -1), (RING2, 7, 1), (RING2, 5, -2), (ROW, 5), (RING2, 6, 2),
    (ROW, 6), (PASS, 3), (RING2, 7, 2), (ROW, 7), (NORM, 0), (FIRST, 0), (NORM, 1), (FIRST, 1), (NORM, 2), (FIRST, 2),
    (SECOND, 0, 0), (SECOND, 0, 1), (SECOND, 0, 2), (SECOND, 0, 3), (SECOND, 1, 0), (SECOND, 1, 1), (SECOND, 1, 2),
    (SECOND, 1, 3), (SECOND, 2, 0), (SECOND, 2, 1), (SECOND, 2, 2), (SECOND, 2, 3), (NORM, 3), (FIRST, 3),
    (SECOND, 3, 0), (SECOND, 3, 1), (RELAY, 0), (SECOND, 3, 2), (SECOND, 3, 3), (RELAY, 1), (RELAY, 2), (RELAY, 3),
    (FINISH, 0), (FINISH, 1), (FINISH, 2), (FINISH, 3),
)
DOWN_ORDER = (
    (OWN,), (PASS, 0), (RING2, 0, 1), (RING1, 1), (RING2, 0, -1), (RING1, -1), (PASS, 1), (RING2, 0, 2),
    (RING2, 1, -1), (RING2, 1, 1), (RING1, 2), (ROW, 0), (RING2, 0, -2), (RING2, 2, 1), (PASS, 2), (RING2, 0, 3),
    (RING2, 2, -1), (RING2, 1, 2), (RING2, 1, -2), (RING2, 3, 1), (ROW, 2), (RING2, 3, -1), (ROW, 1), (RING2, 2, 2),
    (RING2, 0, -3), (PASS, 3), (RING2, 1, 3), (RING2, 2, -2), (RING2, 3, 2), (ROW, 4), (RING2, 1, -3), (NORM, 0),
    (RING2, 2, 3), (RING2, 3, -2), (ROW, 3), (RING2, 0, -4), (RING2, 3, 3), (ROW, 6), (RING2, 2, -3), (RING2, 2, 4),
    (RING2, 1, -4), (RING2, 3, 4), (ROW, 7), (RING2, 3, -3), (ROW, 5), (FIRST, 0), (SECOND, 0, 0), (SECOND, 0, 1),
    (SECOND, 0, 2), (SECOND, 0, 3), (NORM, 1), (FIRST, 1), (SECOND, 1, 0), (SECOND, 1, 1), (SECOND, 1, 2),
    (SECOND, 1, 3), (NORM, 2), (FIRST, 2), (SECOND, 2, 0), (RELAY, 0), (SECOND, 2, 1), (SECOND, 2, 2), (SECOND, 2, 3),
    (NORM, 3), (FIRST, 3), (SECOND, 3, 0), (SECOND, 3, 1), (SECOND, 3, 2), (SECOND, 3, 3), (RELAY, 1), (RELAY, 2),
    (FINISH, 0), (RELAY, 3), (FINISH, 1), (FINISH, 2), (FINISH, 3),
)


def kernel(
    tok_ref, gain_ref, up_ref, down_ref,
    MX, U, D,
    gv, uv, dv, ul, dl, X, N, H, PT, R2, RA, RB,
    loc_sem, dsc_sem,
    u1_s, u1_r, u2_s, u2_r, um_s, um_r,
    d1_s, d1_r, d2_s, d2_r, dm_s, dm_r,
    tx_s, tx_r, rs_s, rs_r,
):
    place = {a: lax.axis_index(a) for a in ("x", "y", "z", "c")}
    x, y, z, c = (place[a] for a in ("x", "y", "z", "c"))
    turn = 1 - 2 * c

    def step(axis, k):
        return lax.rem(place[axis] + k * turn + 2 * SIZE[axis], SIZE[axis])

    def near(axis, k):
        return {axis: step(axis, k)}

    sent = []

    def send(src, dst, ssem, rsem, dev):
        copy = pltpu.make_async_remote_copy(
            src_ref=src, dst_ref=dst, send_sem=ssem, recv_sem=rsem,
            device_id=dev, device_id_type=MESH,
        )
        copy.start()
        sent.append(copy)

    def arrive(dst, ssem, rsem, dev):
        pltpu.make_async_remote_copy(
            src_ref=dst, dst_ref=dst, send_sem=ssem, recv_sem=rsem,
            device_id=dev, device_id_type=MESH,
        ).wait_recv()

    mate = {"c": 1 - c}
    block = lax.div(z, 2)
    far_z = 2 * x + lax.rem(z, 2)
    away = x != block
    leaves = jnp.logical_or(away, c == 0)

    loads = [
        pltpu.make_async_copy(src, dst, loc_sem.at[n])
        for n, (src, dst) in enumerate(((gain_ref, gv), (up_ref, uv), (down_ref, dv), (tok_ref, X.at[3])))
    ]
    for load in loads:
        load.start()

    barrier = pltpu.get_barrier_semaphore()
    for dev in (*(near(a, k) for a in ("x", "y", "z") for k in (1, -1)), mate):
        pl.semaphore_signal(barrier, inc=1, device_id=dev, device_id_type=MESH)

    @pl.when(jnp.logical_and(away, c == 1))
    def _():
        for n in (0, 1):
            pl.semaphore_signal(
                barrier, inc=1, device_id={"x": block, "z": far_z, "c": n}, device_id_type=MESH
            )

    for load in loads[:3]:
        load.wait()
    eye = lax.broadcasted_iota(jnp.int32, (32, 32), 0) == lax.broadcasted_iota(jnp.int32, (32, 32), 1)
    column = jnp.sum(jnp.where(eye, jnp.broadcast_to(gv[...], (32, 32)), 0.0), axis=1, keepdims=True)
    up_mine = (column * uv[...]).astype(jnp.bfloat16)
    ul[...] = up_mine

    @pl.when(c == 0)
    def _():
        U[z, y, 0] = up_mine

    mine = dv[...].astype(jnp.bfloat16)
    dl[...] = mine

    @pl.when(jnp.logical_not(leaves))
    def _():
        D[z, y, c] = mine

    loads[3].wait()

    @pl.when(away)
    def _():
        pl.semaphore_wait(barrier, 8)

    @pl.when(jnp.logical_not(away))
    def _():
        pl.semaphore_wait(barrier, 7)

    def rows(i):
        return pl.ds(i * ROWS, ROWS)

    def stream(events, buf, axes, way1, ways2, s1, r1, s2, r2, sm, rm):

        def piece(k1, k2):
            at = {axes[0]: step(axes[0], k1), axes[1]: step(axes[1], k2)}
            return buf.at[at["z"], at["y"]]

        def hop(way, axis, k, ref, ss, rr):
            for d in (1, -1):
                if (k * d > 0 or k == 0) and k + d in way:
                    n = way.index(k + d) - 1
                    send(ref, ref, ss(n), rr(n), near(axis, -d))

        def hop1(k):
            hop(way1, axes[0], k, piece(k, 0), lambda n: s1.at[n], lambda n: r1.at[n])

        def hop2(i, k):
            hop(ways2[i], axes[1], k, piece(way1[i], k), lambda n: s2.at[i, n], lambda n: r2.at[i, n])

        def own():
            hop1(0)
            hop2(0, 0)

        def take1(i):
            k, n = way1[i], i - 1
            arrive(piece(k, 0), s1.at[n], r1.at[n], near(axes[0], 1))
            hop1(k)
            hop2(i, 0)

        def take2(i, n):
            k = ways2[i][n + 1]
            arrive(piece(way1[i], k), s2.at[i, n], r2.at[i, n], near(axes[1], 1))
            hop2(i, k)

        def row(n):
            zz = step("z", (way1 if axes[0] == "z" else WAY["z", 1])[n])
            send(buf.at[zz], buf.at[zz], sm.at[n], rm.at[zz], mate)

        for i in range(1, len(way1)):
            events[RING1, way1[i]] = lambda i=i: take1(i)
        for i in range(len(way1)):
            for n in range(len(ways2[i]) - 1):
                events[RING2, i, ways2[i][n + 1]] = lambda i=i, n=n: take2(i, n)
        for n in range(8):
            events[ROW, n] = lambda n=n: row(n)

        def complete():
            for n in range(8):
                arrive(buf.at[n], sm.at[n], rm.at[n], mate)

        return own, complete

    up_events, down_events, events = {}, {}, {}
    up_ways = [WAY["y", w] for w in (1, 1, -1, -1) * 2]
    down_ways = [WAY["z", w] for w in (1, 1, -1, -1)]
    up_own, up_complete = stream(up_events, U, "zy", WAY["z", 1], up_ways, u1_s, u1_r, u2_s, u2_r, um_s, um_r)
    down_own, down_complete = stream(down_events, D, "yz", WAY["y", -1], down_ways, d1_s, d1_r, d2_s, d2_r, dm_s, dm_r)

    scatter = pltpu.make_async_remote_copy(
        src_ref=dl, dst_ref=D.at[far_z, y, c], send_sem=dsc_sem.at[2], recv_sem=dsc_sem.at[c],
        device_id={"x": block, "z": far_z, "c": 1}, device_id_type=MESH,
    )
    give = pltpu.make_async_remote_copy(
        src_ref=ul, dst_ref=U.at[z, y, 1], send_sem=dsc_sem.at[3], recv_sem=dsc_sem.at[3],
        device_id={"c": 0}, device_id_type=MESH,
    )

    def scattered(n):
        arrive(D.at[z, y, n], dsc_sem.at[2], dsc_sem.at[n], mate)

    def up_here():
        give.wait_recv()
        up_own()

    def down_here():
        scattered(0)

        @pl.when(away)
        def _():
            scattered(1)

        down_own()

    def token(src, slot, i, k):
        send(X.at[src, rows(i)], X.at[slot, rows(i)], tx_s.at[slot, i], tx_r.at[slot, i], near("x", k))

    def token_in(slot, i):
        arrive(X.at[slot, rows(i)], tx_s.at[slot, i], tx_r.at[slot, i], near("x", 1))

    @pl.when(leaves)
    def _():
        scatter.start()

    def pass_on(i):
        token_in(0, i)
        token(0, 2, i, 1)

    def normalise(i):
        token_in(1, i)
        token_in(2, i)
        owners = (step("x", -1), step("x", 1), step("x", 2), x)

        @pl.loop(0, ROWS // 32)
        def _(b):
            r = pl.ds(pl.multiple_of(i * ROWS + b * 32, 32), 32)
            values = [X[n, r, :].astype(jnp.float32) for n in range(4)]
            total = sum(jnp.sum(v * v, axis=1, keepdims=True) for v in values)
            scale = lax.rsqrt(total * (1.0 / 2048) + 1e-6)
            for v, owner in zip(values, owners):
                N[r, pl.ds(pl.multiple_of(owner * 512, 512), 512)] = (v * scale).astype(jnp.bfloat16)

    def first(i, core):
        if i == 0 and core == 1:
            up_complete()
        for n in range(4):
            w = U[:, :, :, :, n * 256:(n + 1) * 256].reshape(2048, 256)
            before = jnp.dot(N[rows(i), :], w, preferred_element_type=jnp.float32)
            before = jnp.maximum(before, 0.0)
            H[rows(i), n * 256:(n + 1) * 256] = (before * before).astype(jnp.bfloat16)

    def second(i, j, core):
        if i == 0 and j == 0 and core == 0:
            down_complete()
        k, buf, n = ((2, R2, 0), (-1, RB, 1), (1, None, 2), (0, None, 3))[j]
        w = D[pl.ds(2 * step("x", k), 2)].reshape(1024, 512)
        PT[i, j] = jnp.dot(H[rows(i), :], w, preferred_element_type=jnp.float32).astype(jnp.bfloat16)
        if buf is not None:
            send(PT.at[i, j], buf.at[i], rs_s.at[n, i], rs_r.at[n, i], near("x", 1 if j == 0 else -1))

    def relay(i):
        arrive(R2.at[i], rs_s.at[0, i], rs_r.at[0, i], near("x", 1))
        PT[i, 2] = (PT[i, 2].astype(jnp.float32) + R2[i].astype(jnp.float32)).astype(jnp.bfloat16)
        send(PT.at[i, 2], RA.at[i], rs_s.at[2, i], rs_r.at[2, i], near("x", 1))

    def finish(i):
        arrive(RB.at[i], rs_s.at[1, i], rs_r.at[1, i], near("x", 1))
        arrive(RA.at[i], rs_s.at[2, i], rs_r.at[2, i], near("x", 1))
        total = PT[i, 3].astype(jnp.float32) + RA[i].astype(jnp.float32) + RB[i].astype(jnp.float32)
        MX[rows(i), :] = total.astype(jnp.bfloat16)

    for i in range(CHUNKS):
        events[PASS, i] = lambda i=i: pass_on(i)
        events[NORM, i] = lambda i=i: normalise(i)
        events[RELAY, i] = lambda i=i: relay(i)
        events[FINISH, i] = lambda i=i: finish(i)

    def program(core, order):
        todo = events | (down_events if core else up_events) | {(OWN,): down_here if core else up_here}
        for i in range(CHUNKS):
            todo[FIRST, i] = lambda i=i: first(i, core)
            for j in range(4):
                todo[SECOND, i, j] = lambda i=i, j=j: second(i, j, core)
        if core == 1:
            give.start()
        for i in range(CHUNKS):
            token(3, 0, i, 1)
            token(3, 1, i, -1)
        for name in order:
            todo[name]()
        for copy in sent:
            copy.wait_send()
        if core == 1:
            give.wait_send()
        sent.clear()

    @pl.when(c == 0)
    def _():
        program(0, UP_ORDER)

    @pl.when(c == 1)
    def _():
        program(1, DOWN_ORDER)

    @pl.when(leaves)
    def _():
        scatter.wait_send()


def write(mixed_ref, up_ref, down_ref, mixed_out, up_out, down_out, sems):
    copies = [pltpu.make_async_copy(up_ref, up_out, sems.at[0])]
    for n in range(4):
        copies.append(pltpu.make_async_copy(
            down_ref.at[pl.ds(2 * n, 2)], down_out.at[:, :, :, :, pl.ds(n * 512, 512)], sems.at[1 + n]
        ))
    copies.append(pltpu.make_async_copy(mixed_ref, mixed_out, sems.at[5]))
    for copy in copies:
        copy.start()
    for copy in copies:
        copy.wait()


def shards(tokens, norm_gain, up_master, down_master):
    bf = jnp.bfloat16
    f32 = jnp.float32
    sem = pltpu.SemaphoreType.DMA
    vmem = pl.BlockSpec(memory_space=pltpu.VMEM)
    hbm = pl.BlockSpec(memory_space=pltpu.HBM)
    arguments = [
        pltpu.with_memory_space_constraint(v, pltpu.HBM)
        for v in (tokens, norm_gain.reshape(1, 32), up_master, down_master)
    ]
    mixed, up, down = pl.pallas_call(
        kernel,
        out_shape=(
            jax.ShapeDtypeStruct((1024, 512), bf),
            jax.ShapeDtypeStruct((8, 4, 2, 32, 1024), bf),
            jax.ShapeDtypeStruct((8, 4, 2, 64, 512), bf),
        ),
        in_specs=[hbm, hbm, hbm, hbm],
        out_specs=(vmem, vmem, vmem),
        scratch_shapes=[
            pltpu.VMEM((1, 32), f32),
            pltpu.VMEM((32, 1024), f32),
            pltpu.VMEM((64, 512), f32),
            pltpu.VMEM((32, 1024), bf),
            pltpu.VMEM((64, 512), bf),
            pltpu.VMEM((4, 1024, 512), bf),
            pltpu.VMEM((1024, 2048), bf),
            pltpu.VMEM((1024, 1024), bf),
            pltpu.VMEM((CHUNKS, 4, ROWS, 512), bf),
            pltpu.VMEM((CHUNKS, ROWS, 512), bf),
            pltpu.VMEM((CHUNKS, ROWS, 512), bf),
            pltpu.VMEM((CHUNKS, ROWS, 512), bf),
            sem((4,)), sem((4,)),
            sem((7,)), sem((7,)), sem((8, 3)), sem((8, 3)), sem((8,)), sem((8,)),
            sem((3,)), sem((3,)), sem((4, 7)), sem((4, 7)), sem((8,)), sem((8,)),
            sem((3, CHUNKS)), sem((3, CHUNKS)), sem((3, CHUNKS)), sem((3, CHUNKS)),
        ],
        compiler_params=pltpu.CompilerParams(
            collective_id=0, has_side_effects=True, vmem_limit_bytes=40 * 1024 * 1024
        ),
        name="handoff",
    )(*arguments)
    mixed, up, down = pl.pallas_call(
        write,
        out_shape=(
            jax.ShapeDtypeStruct((1024, 512), bf),
            jax.ShapeDtypeStruct((8, 4, 2, 32, 1024), bf),
            jax.ShapeDtypeStruct((2, 4, 2, 64, 2048), bf),
        ),
        in_specs=[vmem, vmem, vmem],
        out_specs=(hbm, hbm, hbm),
        scratch_shapes=[sem((6,))],
        compiler_params=pltpu.CompilerParams(vmem_limit_bytes=16 * 1024 * 1024),
        name="write",
    )(mixed, up, down)
    return mixed, up.reshape(2048, 1024), down.reshape(1024, 2048)


def solution(mesh):
    finer = Mesh(mesh.devices.reshape(8, 4, 2, 4), ("z", "y", "c", "x"))
    return jax.shard_map(
        shards,
        mesh=finer,
        in_specs=(P(FS, "x"), P(FS), P(FS, "x"), P(FS, "x")),
        out_specs=(P(FS, "x"), P(None, "x"), P("x", None)),
        check_vma=False,
    )
```

```python
import jax
import jax.numpy as jnp
from jax import lax
from jax.experimental import pallas as pl
from jax.experimental.pallas import tpu as pltpu
from jax.sharding import Mesh
from jax.sharding import PartitionSpec as P

FS = ("z", "y", "c")
SIZE = {"z": 8, "y": 4, "c": 2, "x": 4}
CHUNKS = 4
ROWS = 256
MESH = pl.DeviceIdType.MESH
WAY = {("y", 1): (0, -1, 1, -2), ("z", 1): (0, -1, 1, -2, 2, -3, 3, -4), ("z", -1): (0, 1, -1, 2, -2, 3, -3, 4), ("y", -1): (0, 1, -1, 2)}
OWN, RING1, RING2, ROW, PASS, NORM, FIRST, SECOND, RELAY, FINISH = range(10)
UP_ORDER = (
    (OWN,), (RING1, -1), (RING1, 1), (RING2, 0, -1), (RING2, 0, 1), (PASS, 0), (RING1, -2), (RING2, 1, -1),
    (RING2, 1, 1), (RING1, 2), (RING2, 2, 1), (RING2, 2, -1), (RING2, 0, -2), (ROW, 0), (RING1, -3), (RING1, 3),
    (RING2, 3, 1), (PASS, 1), (RING2, 3, -1), (RING2, 4, 1), (RING2, 1, -2), (ROW, 1), (RING2, 4, -1), (RING2, 2, 2),
    (ROW, 2), (RING1, -4), (RING2, 5, -1), (RING2, 5, 1), (PASS, 2), (RING2, 6, -1), (RING2, 6, 1), (RING2, 4, -2),
    (ROW, 4), (RING2, 3, 2), (ROW, 3), (RING2, 7, -1), (RING2, 7, 1), (RING2, 5, -2), (ROW, 5), (RING2, 6, 2),
    (ROW, 6), (PASS, 3), (NORM, 0), (RING2, 7, 2), (ROW, 7), (FIRST, 0), (SECOND, 0, 0), (SECOND, 0, 1),
    (SECOND, 0, 2), (SECOND, 0, 3), (NORM, 1), (FIRST, 1), (SECOND, 1, 0), (SECOND, 1, 1), (SECOND, 1, 2),
    (SECOND, 1, 3), (NORM, 2), (FIRST, 2), (SECOND, 2, 0), (SECOND, 2, 1), (SECOND, 2, 2), (SECOND, 2, 3), (RELAY, 0),
    (NORM, 3), (FIRST, 3), (SECOND, 3, 0), (SECOND, 3, 1), (SECOND, 3, 2), (SECOND, 3, 3), (RELAY, 1), (RELAY, 2),
    (RELAY, 3), (FINISH, 0), (FINISH, 1), (FINISH, 2), (FINISH, 3),
)
DOWN_ORDER = (
    (OWN,), (PASS, 0), (RING2, 0, 1), (RING1, 1), (RING2, 0, -1), (RING1, -1), (PASS, 1), (RING2, 0, 2),
    (RING2, 1, -1), (RING2, 1, 1), (RING1, 2), (ROW, 0), (RING2, 0, -2), (RING2, 2, 1), (PASS, 2), (RING2, 0, 3),
    (RING2, 2, -1), (RING2, 1, 2), (RING2, 1, -2), (RING2, 3, 1), (ROW, 2), (RING2, 3, -1), (ROW, 1), (RING2, 2, 2),
    (RING2, 0, -3), (PASS, 3), (RING2, 1, 3), (RING2, 2, -2), (RING2, 3, 2), (ROW, 4), (RING2, 1, -3), (RING2, 2, 3),
    (RING2, 3, -2), (ROW, 3), (NORM, 0), (RING2, 3, 3), (ROW, 6), (RING2, 2, -3), (RING2, 3, -3), (ROW, 5), (FIRST, 0),
    (SECOND, 0, 0), (SECOND, 0, 1), (SECOND, 0, 2), (RING2, 0, -4), (RING2, 2, 4), (RING2, 1, -4), (RING2, 3, 4),
    (ROW, 7), (SECOND, 0, 3), (NORM, 1), (FIRST, 1), (SECOND, 1, 0), (SECOND, 1, 1), (SECOND, 1, 2), (SECOND, 1, 3),
    (NORM, 2), (FIRST, 2), (SECOND, 2, 0), (SECOND, 2, 1), (SECOND, 2, 2), (SECOND, 2, 3), (RELAY, 0), (NORM, 3),
    (FIRST, 3), (SECOND, 3, 0), (SECOND, 3, 1), (SECOND, 3, 2), (SECOND, 3, 3), (RELAY, 1), (RELAY, 2), (RELAY, 3),
    (FINISH, 0), (FINISH, 1), (FINISH, 2), (FINISH, 3),
)


def kernel(
    tok_ref, gain_ref, up_ref, down_ref,
    MX, U, D,
    gv, uv, dv, ul, dl, X, N, H, PT, R2, RA, RB,
    loc_sem, dsc_sem,
    send_sem, ring1_sem, ring2_sem, tx_sem, rs_sem,
):
    place = {a: lax.axis_index(a) for a in ("x", "y", "z", "c")}
    x, y, z, c = (place[a] for a in ("x", "y", "z", "c"))
    turn = 1 - 2 * c

    def step(axis, k):
        return lax.rem(place[axis] + k * turn + 2 * SIZE[axis], SIZE[axis])

    def near(axis, k):
        return {axis: step(axis, k)}

    def copy(src, dst, kind, rsem, dev):
        return pltpu.make_async_remote_copy(
            src_ref=src, dst_ref=dst, send_sem=send_sem.at[kind], recv_sem=rsem,
            device_id=dev, device_id_type=MESH,
        )

    def send(src, dst, kind, rsem, dev):
        copy(src, dst, kind, rsem, dev).start()

    def sent(whole, kind):
        copy(whole, whole, kind, send_sem.at[kind], mate).wait_send()

    def arrive(dst, rsem, dev):
        copy(dst, dst, 0, rsem, dev).wait_recv()

    mate = {"c": 1 - c}
    block = lax.div(z, 2)
    far_z = 2 * x + lax.rem(z, 2)
    away = x != block
    leaves = jnp.logical_or(away, c == 0)

    loads = [
        pltpu.make_async_copy(src, dst, loc_sem.at[n])
        for n, (src, dst) in enumerate(((gain_ref, gv), (up_ref, uv), (down_ref, dv), (tok_ref, X.at[3])))
    ]
    for load in loads:
        load.start()

    barrier = pltpu.get_barrier_semaphore()
    for dev in (*(near(a, k) for a in ("x", "y", "z") for k in (1, -1)), mate):
        pl.semaphore_signal(barrier, inc=1, device_id=dev, device_id_type=MESH)

    @pl.when(jnp.logical_and(away, c == 1))
    def _():
        for n in (0, 1):
            pl.semaphore_signal(
                barrier, inc=1, device_id={"x": block, "z": far_z, "c": n}, device_id_type=MESH
            )

    for load in loads[:3]:
        load.wait()
    eye = lax.broadcasted_iota(jnp.int32, (32, 32), 0) == lax.broadcasted_iota(jnp.int32, (32, 32), 1)
    column = jnp.sum(jnp.where(eye, jnp.broadcast_to(gv[...], (32, 32)), 0.0), axis=1, keepdims=True)
    up_mine = (column * uv[...]).astype(jnp.bfloat16)
    ul[...] = up_mine

    @pl.when(c == 0)
    def _():
        U[z, y, 0] = up_mine

    mine = dv[...].astype(jnp.bfloat16)
    dl[...] = mine

    @pl.when(jnp.logical_not(leaves))
    def _():
        D[z, y, c] = mine

    loads[3].wait()

    @pl.when(away)
    def _():
        pl.semaphore_wait(barrier, 8)

    @pl.when(jnp.logical_not(away))
    def _():
        pl.semaphore_wait(barrier, 7)

    def rows(i):
        return pl.ds(i * ROWS, ROWS)

    def stream(events, buf, axes, way1, ways2):

        def piece(k1, k2):
            at = {axes[0]: step(axes[0], k1), axes[1]: step(axes[1], k2)}
            return buf.at[at["z"], at["y"]]

        wide = len(ways2[0]) - 1

        def hop(way, axis, k, ref, kind, sems):
            for d in (1, -1):
                if (k * d > 0 or k == 0) and k + d in way:
                    send(ref, ref, kind, sems(way.index(k + d) - 1), near(axis, -d))

        def hop1(k):
            hop(way1, axes[0], k, piece(k, 0), 0, lambda n: ring1_sem.at[n])

        def hop2(i, k):
            hop(ways2[i], axes[1], k, piece(way1[i], k), 1, lambda n: ring2_sem.at[i * wide + n])

        def own():
            hop1(0)
            hop2(0, 0)

        def take1(i):
            k, n = way1[i], i - 1
            arrive(piece(k, 0), ring1_sem.at[n], near(axes[0], 1))
            hop1(k)
            hop2(i, 0)

        def take2(i, n):
            k = ways2[i][n + 1]
            arrive(piece(way1[i], k), ring2_sem.at[i * wide + n], near(axes[1], 1))
            hop2(i, k)

        def row(n):
            zz = step("z", WAY["z", 1][n])
            send(buf.at[zz], buf.at[zz], 2, dsc_sem.at[4 + max(n - 1, 0) // 2], mate)

        for i in range(1, len(way1)):
            events[RING1, way1[i]] = lambda i=i: take1(i)
        for i in range(len(way1)):
            for n in range(len(ways2[i]) - 1):
                events[RING2, i, ways2[i][n + 1]] = lambda i=i, n=n: take2(i, n)
        for n in range(8):
            events[ROW, n] = lambda n=n: row(n)

        def complete(distance):
            arrive(buf.at[pl.ds(0, (3, 2, 2, 1)[distance])], dsc_sem.at[4 + distance], mate)

        def all_sent():
            sent(buf.at[pl.ds(0, len(way1) - 1), 0], 0)
            sent(buf.at[pl.ds(0, len(way1) * wide // 4)], 1)
            sent(buf, 2)

        return own, complete, all_sent

    up_events, down_events, events = {}, {}, {}
    up_ways = [WAY["y", w] for w in (1, 1, -1, -1) * 2]
    down_ways = [WAY["z", w] for w in (1, 1, -1, -1)]
    up_own, up_complete, up_sent = stream(up_events, U, "zy", WAY["z", 1], up_ways)
    down_own, down_complete, down_sent = stream(down_events, D, "yz", WAY["y", -1], down_ways)

    scatter = pltpu.make_async_remote_copy(
        src_ref=dl, dst_ref=D.at[far_z, y, c], send_sem=dsc_sem.at[2], recv_sem=dsc_sem.at[c],
        device_id={"x": block, "z": far_z, "c": 1}, device_id_type=MESH,
    )
    give = pltpu.make_async_remote_copy(
        src_ref=ul, dst_ref=U.at[z, y, 1], send_sem=dsc_sem.at[3], recv_sem=dsc_sem.at[3],
        device_id={"c": 0}, device_id_type=MESH,
    )

    def scattered(n):
        arrive(D.at[z, y, n], dsc_sem.at[n], mate)

    def up_here():
        give.wait_recv()
        up_own()

    def down_here():
        scattered(0)

        @pl.when(away)
        def _():
            scattered(1)

        down_own()

    def token(src, slot, i, k):
        send(X.at[src, rows(i)], X.at[slot, rows(i)], 3, tx_sem.at[slot, i], near("x", k))

    def token_in(slot, i):
        arrive(X.at[slot, rows(i)], tx_sem.at[slot, i], near("x", 1))

    @pl.when(leaves)
    def _():
        scatter.start()

    def pass_on(i):
        token_in(0, i)
        token(0, 2, i, 1)

    def normalise(i):
        token_in(1, i)
        token_in(2, i)
        owners = (step("x", -1), step("x", 1), step("x", 2), x)

        @pl.loop(0, ROWS // 32)
        def _(b):
            r = pl.ds(pl.multiple_of(i * ROWS + b * 32, 32), 32)
            values = [X[n, r, :].astype(jnp.float32) for n in range(4)]
            total = sum(jnp.sum(v * v, axis=1, keepdims=True) for v in values)
            scale = lax.rsqrt(total * (1.0 / 2048) + 1e-6)
            for v, owner in zip(values, owners):
                N[r, pl.ds(pl.multiple_of(owner * 512, 512), 512)] = (v * scale).astype(jnp.bfloat16)

    def first(i, core):
        if i == 0 and core == 1:
            for distance in range(4):
                up_complete(distance)
        for n in range(4):
            w = U[:, :, :, :, n * 256:(n + 1) * 256].reshape(2048, 256)
            before = jnp.dot(N[rows(i), :], w, preferred_element_type=jnp.float32)
            before = jnp.maximum(before, 0.0)
            H[rows(i), n * 256:(n + 1) * 256] = (before * before).astype(jnp.bfloat16)

    lean = 1 - 2 * lax.rem(z, 2)

    def second(i, j, core):
        if i == 0 and core == 0:
            down_complete(j)
        cc = lax.rem(block + (0, -1, 1, 2)[j] * lean + 4, 4)
        hops = lax.rem((cc - x) * turn + 8, 4)
        w = D[pl.ds(2 * cc, 2)].reshape(1024, 512)
        PT[i, hops] = jnp.dot(H[rows(i), :], w, preferred_element_type=jnp.float32).astype(jnp.bfloat16)

        @pl.when(hops == 2)
        def _():
            send(PT.at[i, 2], R2.at[i], 4, rs_sem.at[0, i], near("x", 1))

        @pl.when(hops == 3)
        def _():
            send(PT.at[i, 3], RB.at[i], 4, rs_sem.at[1, i], near("x", -1))

    def relay(i):
        arrive(R2.at[i], rs_sem.at[0, i], near("x", 1))
        PT[i, 1] = (PT[i, 1].astype(jnp.float32) + R2[i].astype(jnp.float32)).astype(jnp.bfloat16)
        send(PT.at[i, 1], RA.at[i], 4, rs_sem.at[2, i], near("x", 1))

    def finish(i):
        arrive(RB.at[i], rs_sem.at[1, i], near("x", 1))
        arrive(RA.at[i], rs_sem.at[2, i], near("x", 1))
        total = PT[i, 0].astype(jnp.float32) + RA[i].astype(jnp.float32) + RB[i].astype(jnp.float32)
        MX[rows(i), :] = total.astype(jnp.bfloat16)

    for i in range(CHUNKS):
        events[PASS, i] = lambda i=i: pass_on(i)
        events[NORM, i] = lambda i=i: normalise(i)
        events[RELAY, i] = lambda i=i: relay(i)
        events[FINISH, i] = lambda i=i: finish(i)

    def program(core, order):
        todo = events | (down_events if core else up_events) | {(OWN,): down_here if core else up_here}
        for i in range(CHUNKS):
            todo[FIRST, i] = lambda i=i: first(i, core)
            for j in range(4):
                todo[SECOND, i, j] = lambda i=i, j=j: second(i, j, core)
        if core == 1:
            give.start()
        for i in range(CHUNKS):
            token(3, 0, i, 1)
            token(3, 1, i, -1)
        for name in order:
            todo[name]()
        sent(X.at[pl.ds(0, 3)], 3)
        sent(PT.at[pl.ds(0, 3)], 4)
        if core == 1:
            down_sent()
            give.wait_send()
        else:
            up_sent()

    @pl.when(c == 0)
    def _():
        program(0, UP_ORDER)

    @pl.when(c == 1)
    def _():
        program(1, DOWN_ORDER)

    @pl.when(leaves)
    def _():
        scatter.wait_send()


def write(mixed_ref, up_ref, down_ref, mixed_out, up_out, down_out, sems):
    copies = [pltpu.make_async_copy(mixed_ref, mixed_out, sems.at[8])]
    for n in range(4):
        two = pl.ds(2 * n, 2)
        copies.append(pltpu.make_async_copy(up_ref.at[two], up_out.at[two], sems.at[n]))
        copies.append(pltpu.make_async_copy(
            down_ref.at[two], down_out.at[:, :, :, :, pl.ds(n * 512, 512)], sems.at[4 + n]
        ))
    for copy in copies:
        copy.start()
    for copy in copies:
        copy.wait()


def shards(tokens, norm_gain, up_master, down_master):
    bf = jnp.bfloat16
    f32 = jnp.float32
    sem = pltpu.SemaphoreType.DMA
    vmem = pl.BlockSpec(memory_space=pltpu.VMEM)
    hbm = pl.BlockSpec(memory_space=pltpu.HBM)
    arguments = [
        pltpu.with_memory_space_constraint(v, pltpu.HBM)
        for v in (tokens, norm_gain.reshape(1, 32), up_master, down_master)
    ]
    mixed, up, down = pl.pallas_call(
        kernel,
        out_shape=(
            jax.ShapeDtypeStruct((1024, 512), bf),
            jax.ShapeDtypeStruct((8, 4, 2, 32, 1024), bf),
            jax.ShapeDtypeStruct((8, 4, 2, 64, 512), bf),
        ),
        in_specs=[hbm, hbm, hbm, hbm],
        out_specs=(vmem, vmem, vmem),
        scratch_shapes=[
            pltpu.VMEM((1, 32), f32),
            pltpu.VMEM((32, 1024), f32),
            pltpu.VMEM((64, 512), f32),
            pltpu.VMEM((32, 1024), bf),
            pltpu.VMEM((64, 512), bf),
            pltpu.VMEM((4, 1024, 512), bf),
            pltpu.VMEM((1024, 2048), bf),
            pltpu.VMEM((1024, 1024), bf),
            pltpu.VMEM((CHUNKS, 4, ROWS, 512), bf),
            pltpu.VMEM((CHUNKS, ROWS, 512), bf),
            pltpu.VMEM((CHUNKS, ROWS, 512), bf),
            pltpu.VMEM((CHUNKS, ROWS, 512), bf),
            sem((4,)), sem((8,)), sem((5,)), sem((7,)), sem((28,)), sem((3, CHUNKS)), sem((3, CHUNKS)),
        ],
        compiler_params=pltpu.CompilerParams(
            collective_id=0, has_side_effects=True, vmem_limit_bytes=40 * 1024 * 1024
        ),
        name="handoff",
    )(*arguments)
    mixed, up, down = pl.pallas_call(
        write,
        out_shape=(
            jax.ShapeDtypeStruct((1024, 512), bf),
            jax.ShapeDtypeStruct((8, 4, 2, 32, 1024), bf),
            jax.ShapeDtypeStruct((2, 4, 2, 64, 2048), bf),
        ),
        in_specs=[vmem, vmem, vmem],
        out_specs=(hbm, hbm, hbm),
        scratch_shapes=[sem((9,))],
        compiler_params=pltpu.CompilerParams(vmem_limit_bytes=16 * 1024 * 1024),
        name="write",
    )(mixed, up, down)
    return mixed, up.reshape(2048, 1024), down.reshape(1024, 2048)


def solution(mesh):
    finer = Mesh(mesh.devices.reshape(8, 4, 2, 4), ("z", "y", "c", "x"))
    return jax.shard_map(
        shards,
        mesh=finer,
        in_specs=(P(FS, "x"), P(FS), P(FS, "x"), P(FS, "x")),
        out_specs=(P(FS, "x"), P(None, "x"), P("x", None)),
        check_vma=False,
    )
```
